128 devices in a mesh: ep: 128 (over z, y, x, core).
Axes of the slice: x: 4, y: 4, z: 4, core: 2. Of those that a mesh axis runs over, the one named last changes fastest.
Arguments:
- tokens: bfloat16 [2048, 2048], P('ep'), may hold values from -6 to 6
- recurrent_state: float32 [2048, 16, 4096], P('ep'), may hold values from -8 to 8
- first_gain: float32 [2048], replicated, may hold values from 0.1 to 1.9
- w_receptance: bfloat16 [2048, 1024], P('ep'), may hold values from -0.125 to 0.125
- w_key: bfloat16 [2048, 1024], P('ep'), may hold values from -0.125 to 0.125
- w_value: bfloat16 [2048, 1024], P('ep'), may hold values from -0.125 to 0.125
- decay_down: bfloat16 [2048, 64], replicated, may hold values from -0.125 to 0.125
- decay_up: bfloat16 [64, 1024], replicated, may hold values from -0.75 to 0.75
- decay_base: float32 [1024], replicated, may hold values from -4 to 1
- rate_down: bfloat16 [2048, 64], replicated, may hold values from -0.125 to 0.125
- rate_up: bfloat16 [64, 1024], replicated, may hold values from -0.75 to 0.75
- rate_base: float32 [1024], replicated, may hold values from -5 to 5
- key_scale: float32 [1024], replicated, may hold values from 0.25 to 4
- head_gain: float32 [1024], replicated, may hold values from 0.1 to 1.9
- w_output: bfloat16 [1024, 2048], replicated, may hold values from -0.1875 to 0.1875
- second_gain: float32 [2048], replicated, may hold values from 0.1 to 1.9
- shared_gate: bfloat16 [2048, 512], replicated, may hold values from -0.125 to 0.125
- shared_up: bfloat16 [2048, 512], replicated, may hold values from -0.125 to 0.125
- shared_down: bfloat16 [512, 2048], replicated, may hold values from -0.25 to 0.25
- expert_gate: bfloat16 [128, 2048, 512], P('ep'), may hold values from -0.125 to 0.125
- expert_up: bfloat16 [128, 2048, 512], P('ep'), may hold values from -0.125 to 0.125
- expert_down: bfloat16 [128, 512, 2048], P('ep'), may hold values from -0.25 to 0.25
- routes: int32 [2048, 4], replicated, may hold values from 0 to 127, all different within a row; in each aligned block of 16 rows (0 to 15, 16 to 31, ...) at most 4 rows name the same one
- route_weights: float32 [2048, 4], replicated, may hold values from 0.1 to 1
Outputs:
- new_tokens: bfloat16 [2048, 2048], P('ep')
- new_state: float32 [2048, 16, 4096], P('ep')
The draws below stay inside these ranges and needn't reach their ends.
Inputs may be any that keep to these rules, and one draw needn't show every extreme that they name: `routes`: each row names 4 different experts. In the rows of one device no expert is named by more than 4 rows, a bound that some block reaches of them.
All inputs are finite; a program needn't handle non-finite values.
Results may differ from the reference program's by a relative error of at most 0.015.
Values may be sent and summed in bfloat16 or wider, within the bound.
No kernel may reach another device: no remote copies, remote signals or barrier semaphores. Data moves between devices by JAX's collectives and lax.ppermute only.
A program may use at most 128 MiB of HBM per device.

```python
import math
import jax
import jax.numpy as jnp
import numpy as np
from jax import lax

D = 2048
HEADS = 16
HEAD = 64
DECAY_RANK = 64
RATE_RANK = 64
EXPERT_W = 512
SHARED_W = 512
TOPK = 4
MOST = 4
SEQ_DEV = 16
MIX = 1024
STATE = 4096
EXPERTS = 128
TOKENS = 2048
N_EP = 128


def block_levels(key, dims, split, least, largest):
    def one(position, blocks):
        heights = jax.random.uniform(jax.random.fold_in(jax.random.fold_in(key, 6), position), (blocks,), jnp.float32, least / len(split), largest / len(split))
        return jnp.repeat(jnp.exp(heights), dims[position] // blocks).reshape((-1,) + (1,) * (len(dims) - position - 1))

    level = one(*split[0])
    for cut in split[1:]:
        level = level * one(*cut)
    return level


def assign_block(rng, own, number, rows, count, top, most, skew):
    sequence = jax.random.permutation(rng, count)
    heavy_load, common = load_shares(count, rows * top, most, skew, True), load_shares(count, rows * top, most, skew, False)
    places = jnp.arange(count)

    def named(sizes, rotation):
        used = int((sizes > 0).sum())
        fixed = max(1, used // 4)
        shifted = fixed + (places - fixed + rotation * (used - fixed)) % max(1, count - fixed)
        return jnp.zeros((count,), jnp.int32).at[sequence[jnp.where(places < fixed, places, shifted)]].set(jnp.asarray(sizes, jnp.int32))

    sizes = jnp.where(number % 4 == 0, named(heavy_load, number // 4), named(common, number - number // 4 - 1))
    mixed = jax.random.permutation(jax.random.fold_in(own, 3), count)
    donor, sink = mixed[0:count // 2 * 2:2], mixed[1:count // 2 * 2:2]
    slack = jnp.minimum(sizes[donor] - 1, most - sizes[sink]) // 2
    slack = jnp.where((donor == sequence[0]) | (sink == sequence[0]) | (sizes[sink] == 0), 0, jnp.maximum(slack, 0))
    shifted = jax.random.randint(jax.random.fold_in(own, 4), (count // 2,), 0, 1 << 20) % (slack + 1)
    sizes = sizes.at[donor].add(-shifted).at[sink].add(shifted)
    labels = jnp.searchsorted(jnp.cumsum(sizes), jnp.arange(rows * top), side="right").astype(jnp.int32)
    listing = labels.reshape(top, rows).T
    listing = listing[jax.random.permutation(jax.random.fold_in(own, 1), rows)]
    rotation = jax.random.randint(jax.random.fold_in(own, 2), (rows, 1), 0, top)
    return jnp.take_along_axis(listing, (jnp.arange(top)[None, :] + rotation) % top, axis=1)


def load_shares(amount, total, bound, skew, full):
    loads = [(1 << 20) // math.isqrt(rank ** skew) + 1 for rank in range(1, amount + 1)]
    largest = bound if full else min(bound, max(-(-total // amount), total * loads[0] // sum(loads)))
    least = 1 if total - largest >= amount - 1 else 0
    given, surplus = [largest] + [least] * (amount - 1), total - largest - least * (amount - 1)
    while surplus > 0:
        candidates = [i for i in range(1, amount) if given[i] < largest] or [i for i in range(1, amount) if given[i] < bound]
        pool, left = sum([loads[i] for i in candidates]), surplus
        for i in candidates:
            addition = min(bound - given[i], max(1, left * loads[i] // pool), surplus)
            given[i] = given[i] + addition
            surplus = surplus - addition
    return np.array(given)


def bell_draw(own_key, dims, scale, most, split=(), kind=jnp.bfloat16):
    factor_of = block_levels(own_key, dims, split, -0.22, 0.18) if split else 1.0
    values = jax.random.normal(own_key, dims, jnp.float32) * scale * factor_of
    return jnp.minimum(jnp.maximum(values, -most), most).astype(kind)


def setup_inputs(seed: int = 0) -> dict:
    arg_keys = jax.random.split(jax.random.key(seed), 25)
    tokens = bell_draw(arg_keys[0], (TOKENS, D), 1.0, 6.0, ((0, 128),))
    recurrent_state = bell_draw(arg_keys[1], (TOKENS, HEADS, STATE), 2.0, 8.0, ((0, 128),), jnp.float32)
    first_gain = jnp.clip(1.0 + 0.18 * jax.random.normal(arg_keys[2], (D,), jnp.float32), 0.1, 1.9)
    w_receptance = bell_draw(arg_keys[3], (D, MIX), D ** -0.5, 0.125, ((0, 128),))
    w_key = bell_draw(arg_keys[4], (D, MIX), D ** -0.5, 0.125, ((0, 128),))
    w_value = bell_draw(arg_keys[5], (D, MIX), D ** -0.5, 0.125, ((0, 128),))
    decay_down = bell_draw(arg_keys[6], (D, DECAY_RANK), D ** -0.5, 0.125)
    decay_up = bell_draw(arg_keys[7], (DECAY_RANK, MIX), DECAY_RANK ** -0.5, 0.75)
    decay_base = jnp.clip(jax.random.uniform(arg_keys[8], (MIX,), jnp.float32, -4.0, 1.0), -4.0, 1.0)
    rate_down = bell_draw(arg_keys[9], (D, RATE_RANK), D ** -0.5, 0.125)
    rate_up = bell_draw(arg_keys[10], (RATE_RANK, MIX), RATE_RANK ** -0.5, 0.75)
    rate_base = bell_draw(arg_keys[11], (MIX,), 2.0, 5.0, (), jnp.float32)
    key_scale = jnp.clip(jnp.exp(jax.random.uniform(arg_keys[12], (MIX,), jnp.float32, math.log(0.25), math.log(4.0))), 0.25, 4.0)
    head_gain = jnp.clip(1.0 + 0.18 * jax.random.normal(arg_keys[13], (MIX,), jnp.float32), 0.1, 1.9)
    w_output = bell_draw(arg_keys[14], (MIX, D), MIX ** -0.5, 0.1875)
    second_gain = jnp.clip(1.0 + 0.18 * jax.random.normal(arg_keys[15], (D,), jnp.float32), 0.1, 1.9)
    shared_gate = bell_draw(arg_keys[16], (D, SHARED_W), D ** -0.5, 0.125)
    shared_up = bell_draw(arg_keys[17], (D, SHARED_W), D ** -0.5, 0.125)
    shared_down = bell_draw(arg_keys[18], (SHARED_W, D), SHARED_W ** -0.5, 0.25)
    expert_gate = bell_draw(arg_keys[19], (EXPERTS, D, EXPERT_W), D ** -0.5, 0.125, ((0, 128),))
    expert_up = bell_draw(arg_keys[20], (EXPERTS, D, EXPERT_W), D ** -0.5, 0.125, ((0, 128),))
    expert_down = bell_draw(arg_keys[21], (EXPERTS, EXPERT_W, D), EXPERT_W ** -0.5, 0.25, ((0, 128),))
    routes_keys = jax.random.split(jax.random.fold_in(arg_keys[22], 1), TOKENS // SEQ_DEV)
    routes_turns = jax.random.permutation(jax.random.fold_in(arg_keys[22], 3), TOKENS // SEQ_DEV)
    routes = jax.vmap(lambda own, number: assign_block(jax.random.fold_in(arg_keys[22], 2), own, number, SEQ_DEV, EXPERTS, TOPK, MOST, 2))(routes_keys, routes_turns).reshape((TOKENS, TOPK))
    route_weights = jnp.clip(jax.random.uniform(arg_keys[23], (TOKENS, TOPK), jnp.float32, 0.1, 1.0), 0.1, 1.0)
    return {"tokens": tokens, "recurrent_state": recurrent_state, "first_gain": first_gain, "w_receptance": w_receptance, "w_key": w_key, "w_value": w_value, "decay_down": decay_down, "decay_up": decay_up, "decay_base": decay_base, "rate_down": rate_down, "rate_up": rate_up, "rate_base": rate_base, "key_scale": key_scale, "head_gain": head_gain, "w_output": w_output, "second_gain": second_gain, "shared_gate": shared_gate, "shared_up": shared_up, "shared_down": shared_down, "expert_gate": expert_gate, "expert_up": expert_up, "expert_down": expert_down, "routes": routes, "route_weights": route_weights}


NORM_EPS = 1e-06
GROUP_EPS = 0.00064

def rms_scale(inputs, gain):
    widened = inputs.astype(jnp.float32)
    return widened * lax.rsqrt(lax.optimization_barrier(jnp.mean(widened * widened, axis=-1, keepdims=True)) + NORM_EPS) * gain

def gated_units(inputs, gate_weight, up_weight):
    gate_part = jnp.dot(inputs, gate_weight, preferred_element_type=jnp.float32)
    up_part = jnp.dot(inputs, up_weight, preferred_element_type=jnp.float32)
    return (jax.nn.silu(gate_part) * up_part).astype(jnp.bfloat16)

def mix_heads(normed, receptance, key_rows, value_rows, state_old, decay_down, decay_up, decay_base, rate_down, rate_up, rate_base, key_scale, head_gain):
    count_rows = normed.shape[0]
    heads_count = state_old.shape[1]
    decay_low = jnp.tanh(jnp.dot(normed, decay_down, preferred_element_type=jnp.float32)).astype(jnp.bfloat16)
    decay_pre = decay_base + jnp.dot(decay_low, decay_up, preferred_element_type=jnp.float32)
    decay_rate = jnp.exp(-jnp.exp(-jax.nn.softplus(-decay_pre) - 0.5))
    rate_low = jnp.dot(normed, rate_down, preferred_element_type=jnp.float32).astype(jnp.bfloat16)
    learn_rate = jax.nn.sigmoid(rate_base + jnp.dot(rate_low, rate_up, preferred_element_type=jnp.float32))

    def by_head(inputs):
        return inputs.astype(jnp.float32).reshape(count_rows, heads_count, HEAD)
    reader = by_head(receptance)
    key_heads = by_head(key_rows)
    value_heads = by_head(value_rows)
    decay_heads = by_head(decay_rate)
    learn_heads = by_head(learn_rate)
    scaled = key_heads * key_scale.reshape(heads_count, HEAD)
    direction = scaled / jnp.sqrt(lax.optimization_barrier(jnp.sum(scaled * scaled, axis=-1, keepdims=True)) + 1.0)
    state_prev = state_old.reshape(count_rows, heads_count, HEAD, HEAD)
    removed = lax.optimization_barrier(jnp.sum(state_prev * direction[:, :, None, :], axis=-1))
    state_next = state_prev * decay_heads[:, :, None, :] - removed[..., None] * (direction * learn_heads)[:, :, None, :] + value_heads[..., None] * key_heads[:, :, None, :]
    readout = lax.optimization_barrier(jnp.sum(state_next * reader[:, :, None, :], axis=-1))
    centre = lax.optimization_barrier(jnp.mean(readout, axis=-1, keepdims=True))
    spread = lax.optimization_barrier(jnp.mean(jnp.square(readout - centre), axis=-1, keepdims=True))
    normalized = ((readout - centre) * lax.rsqrt(spread + GROUP_EPS)).reshape(count_rows, heads_count * HEAD)
    normalized = normalized * head_gain
    return (normalized.astype(jnp.bfloat16), state_next.reshape(count_rows, heads_count, HEAD * HEAD))

def routed_mix(second, routes, route_weights, expert_gate, expert_up, expert_down):
    span_rows = 64
    count_rows = second.shape[0]
    width = second.shape[1]
    experts_all = expert_gate.shape[0]
    flat_expert = routes.reshape(-1).astype(jnp.int32)
    assigned = flat_expert.shape[0]
    flat_token = jnp.arange(assigned, dtype=jnp.int32) // TOPK
    flat_weight = route_weights.reshape(-1)
    ordering = jnp.argsort(flat_expert, stable=True)
    sorted_expert = flat_expert[ordering]
    counts = lax.optimization_barrier(jnp.sum((flat_expert[None, :] == jnp.arange(experts_all, dtype=jnp.int32)[:, None]).astype(jnp.int32), axis=1)).astype(jnp.int32)
    padded = (counts + span_rows - 1) // span_rows * span_rows
    start_sorted = (jnp.cumsum(counts) - counts).astype(jnp.int32)
    end_padded = jnp.cumsum(padded).astype(jnp.int32)
    start_padded = (end_padded - padded).astype(jnp.int32)
    target = (start_padded[sorted_expert] + (jnp.arange(assigned, dtype=jnp.int32) - start_sorted[sorted_expert])).astype(jnp.int32)
    total_rows = (assigned + experts_all * (span_rows - 1) + span_rows - 1) // span_rows * span_rows
    total_spans = total_rows // span_rows
    row_token = jnp.full((total_rows,), count_rows, jnp.int32).at[target].set(flat_token[ordering])
    row_weight = jnp.zeros((total_rows,), jnp.float32).at[target].set(flat_weight[ordering])
    span_expert = jnp.minimum(jnp.searchsorted(end_padded, jnp.arange(total_spans, dtype=jnp.int32) * span_rows, side='right'), experts_all - 1).astype(jnp.int32)
    table = jnp.concatenate([second, jnp.zeros((1, width), second.dtype)], axis=0)

    def one_span(inputs):
        which, token_ids, weights = inputs
        picked = table[token_ids]
        hidden = gated_units(picked, expert_gate[which], expert_up[which])
        result = jnp.dot(hidden, expert_down[which], preferred_element_type=jnp.float32).astype(jnp.bfloat16)
        return result.astype(jnp.float32) * weights[:, None]
    span_out = lax.map(one_span, (span_expert, row_token.reshape(total_spans, span_rows), row_weight.reshape(total_spans, span_rows)))
    summed = jnp.zeros((count_rows + 1, width), jnp.float32).at[row_token].add(span_out.reshape(total_rows, width))
    return summed[:count_rows]

def reference(tokens, recurrent_state, first_gain, w_receptance, w_key, w_value, decay_down, decay_up, decay_base, rate_down, rate_up, rate_base, key_scale, head_gain, w_output, second_gain, shared_gate, shared_up, shared_down, expert_gate, expert_up, expert_down, routes, route_weights):
    normed = rms_scale(tokens, first_gain).astype(jnp.bfloat16)
    receptance = jnp.dot(normed, w_receptance, preferred_element_type=jnp.float32).astype(jnp.bfloat16)
    key_rows = jnp.dot(normed, w_key, preferred_element_type=jnp.float32).astype(jnp.bfloat16)
    value_rows = jnp.dot(normed, w_value, preferred_element_type=jnp.float32).astype(jnp.bfloat16)

    def per_block(group):
        return mix_heads(group[0], group[1], group[2], group[3], group[4], decay_down, decay_up, decay_base, rate_down, rate_up, rate_base, key_scale, head_gain)
    grouped = (normed.reshape(N_EP, SEQ_DEV, D), receptance.reshape(N_EP, SEQ_DEV, MIX), key_rows.reshape(N_EP, SEQ_DEV, MIX), value_rows.reshape(N_EP, SEQ_DEV, MIX), recurrent_state.reshape(N_EP, SEQ_DEV, HEADS, STATE))
    mixed, new_state = lax.map(per_block, grouped)
    mixed = mixed.reshape(TOKENS, MIX)
    new_state = new_state.reshape(TOKENS, HEADS, STATE)
    residual = (tokens.astype(jnp.float32) + jnp.dot(mixed, w_output, preferred_element_type=jnp.float32)).astype(jnp.bfloat16)
    second = rms_scale(residual, second_gain).astype(jnp.bfloat16)
    shared = jnp.dot(gated_units(second, shared_gate, shared_up), shared_down, preferred_element_type=jnp.float32)
    routed = routed_mix(second, routes, route_weights, expert_gate, expert_up, expert_down)
    new_tokens = (residual.astype(jnp.float32) + shared + routed).astype(jnp.bfloat16)
    return (new_tokens, new_state)
```

```python
import jax
import jax.numpy as jnp
from jax import lax
from jax.experimental import pallas as pl
from jax.experimental.pallas import tpu as pltpu
from jax.sharding import PartitionSpec as P

HEAD = 64
MOST = 4
HALVES = 2
NORM_EPS = 1e-06
GROUP_EPS = 0.00064
BF = jnp.bfloat16
F32 = jnp.float32


def sent_together(arrays, axis, dim, along):
    ends, at = ([], 0)
    for a in arrays[:-1]:
        at += a.shape[along]
        ends.append(at)
    both = jnp.concatenate(arrays, axis=along)
    return tuple(jnp.split(lax.all_gather(both, axis, axis=dim, tiled=True), ends, axis=along))


def rms_scale(inputs, gain):
    widened = inputs.astype(F32)
    return (
        widened * lax.rsqrt(jnp.mean(widened * widened, axis=-1, keepdims=True) + NORM_EPS) * gain
    )


def dot32(a, b):
    return jnp.dot(a, b, preferred_element_type=F32)


def gated_units(inputs, gate_weight, up_weight):
    return (jax.nn.silu(dot32(inputs, gate_weight)) * dot32(inputs, up_weight)).astype(BF)


def high_low(x):
    high = x.astype(BF)
    return high, (x - high.astype(F32)).astype(BF)


def mix_kernel(vec_ref, gain_ref, state_ref, spread_ref, fold_ref, mixed_ref, next_ref):
    rows = state_ref.shape[0]
    heads = state_ref.shape[1]
    lanes = state_ref.shape[2]
    chunk = 1024
    both = rows * heads

    def part(i):
        return vec_ref[:, i].reshape(both, HEAD)

    def twice(x):
        return jnp.concatenate([x, x], axis=1)

    reader, key, value, decay, learn, scale = (part(i) for i in range(6))
    scaled = key * scale
    direction = scaled / jnp.sqrt(jnp.sum(scaled * scaled, axis=-1, keepdims=True) + 1.0)
    decay2 = twice(decay)
    key2 = twice(key)
    reader2 = twice(reader)
    dir2 = twice(direction)
    taken2 = twice(direction * learn)
    removed = jnp.zeros((both, HEAD), F32)
    for c in range(lanes // chunk):
        pieces = []
        for j in range(chunk // 128):
            at = c * chunk + j * 128
            pieces.append(state_ref[:, :, at : at + 128].reshape(both, 128) * dir2)
        product = jnp.concatenate(pieces, axis=1)
        high, low = high_low(product)
        fold = fold_ref[c * chunk : (c + 1) * chunk, :]
        removed = removed + dot32(high, fold) + dot32(low, fold)
    high, low = high_low(removed)
    known = jnp.concatenate([high, low], axis=1)
    value = value.astype(BF)
    readout = jnp.zeros((both, HEAD), F32)
    for c in range(lanes // chunk):
        spread = spread_ref[:, c * chunk : (c + 1) * chunk]
        removed_wide = dot32(known, jnp.concatenate([spread, spread], axis=0))
        value_wide = dot32(value, spread)
        pieces = []
        for j in range(chunk // 128):
            at = c * chunk + j * 128
            sub = slice(j * 128, j * 128 + 128)
            state = (
                state_ref[:, :, at : at + 128].reshape(both, 128) * decay2
                - removed_wide[:, sub] * taken2
                + value_wide[:, sub] * key2
            )
            next_ref[:, :, at : at + 128] = state.reshape(rows, heads, 128)
            pieces.append(state * reader2)
        product = jnp.concatenate(pieces, axis=1)
        high, low = high_low(product)
        fold = fold_ref[c * chunk : (c + 1) * chunk, :]
        readout = readout + dot32(high, fold) + dot32(low, fold)
    centre = jnp.mean(readout, axis=-1, keepdims=True)
    apart = readout - centre
    spread_var = jnp.mean(apart * apart, axis=-1, keepdims=True)
    gain = jnp.broadcast_to(gain_ref[...][None], (rows, heads, HEAD)).reshape(both, HEAD)
    mixed = apart * lax.rsqrt(spread_var + GROUP_EPS) * gain
    mixed_ref[...] = mixed.reshape(rows, heads, HEAD)


def mix_heads(vectors, head_gain, state_old):
    count, heads, lanes = state_old.shape
    rows = 4
    lane = jnp.arange(lanes, dtype=jnp.int32)
    entry = jnp.arange(HEAD, dtype=jnp.int32)
    spread = (entry[:, None] == lane[None, :] // HEAD).astype(BF)
    fold = (lane[:, None] // HEAD == entry[None, :]).astype(BF)
    return pl.pallas_call(
        mix_kernel,
        grid=(count // rows,),
        in_specs=[
            pl.BlockSpec((rows, 6, heads, HEAD), lambda i: (i, 0, 0, 0)),
            pl.BlockSpec((heads, HEAD), lambda i: (0, 0)),
            pl.BlockSpec((rows, heads, lanes), lambda i: (i, 0, 0)),
            pl.BlockSpec((HEAD, lanes), lambda i: (0, 0)),
            pl.BlockSpec((lanes, HEAD), lambda i: (0, 0)),
        ],
        out_specs=[
            pl.BlockSpec((rows, heads, HEAD), lambda i: (i, 0, 0)),
            pl.BlockSpec((rows, heads, lanes), lambda i: (i, 0, 0)),
        ],
        out_shape=[
            jax.ShapeDtypeStruct((count, heads, HEAD), F32),
            jax.ShapeDtypeStruct((count, heads, lanes), F32),
        ],
        name="mix",
    )(vectors, head_gain.reshape(heads, HEAD), state_old, spread, fold)


def per_device(
    tokens,
    recurrent_state,
    first_gain,
    w_receptance,
    w_key,
    w_value,
    decay_down,
    decay_up,
    decay_base,
    rate_down,
    rate_up,
    rate_base,
    key_scale,
    head_gain,
    w_output,
    second_gain,
    shared_gate,
    shared_up,
    shared_down,
    expert_gate,
    expert_up,
    expert_down,
    routes,
    route_weights,
):
    rows, width = tokens.shape
    heads = recurrent_state.shape[1]
    mix = w_key.shape[1]
    half = width // HALVES
    devices = lax.axis_size("ep")
    my_expert = lax.axis_index("ep")

    own_routes = lax.dynamic_slice_in_dim(routes, my_expert * rows, rows, 0)
    own_weights = lax.dynamic_slice_in_dim(route_weights, my_expert * rows, rows, 0)
    place = jnp.arange(devices * MOST * HALVES, dtype=jnp.int32)
    named = own_routes[:, :, None] == (place // (MOST * HALVES))[None, None, :]
    weight = jnp.sum(jnp.where(named, own_weights[:, :, None], 0.0), axis=1)
    named = jnp.any(named, axis=1)
    order = jnp.arange(rows, dtype=jnp.int32)
    before = (order[None, :] < order[:, None]).astype(BF)
    slot = dot32(before, named.astype(BF))
    chosen = named & (slot == (place % MOST)[None, :].astype(F32))
    side = (place // MOST) % HALVES
    picks = [chosen & (side == h)[None, :] for h in range(HALVES)]
    pick = jnp.concatenate(picks, axis=0).astype(BF)
    weigh_high, weigh_low = high_low(
        jnp.concatenate([jnp.where(p, weight, 0.0) for p in picks], axis=0)
    )
    weigh = jnp.concatenate([weigh_high, weigh_low], axis=0)

    normed = rms_scale(tokens, first_gain).astype(BF)
    decay_low = jnp.tanh(dot32(normed, decay_down)).astype(BF)
    decay_pre = decay_base + dot32(decay_low, decay_up)
    decay_rate = jnp.exp(-jnp.exp(-jax.nn.softplus(-decay_pre) - 0.5))
    rate_low = dot32(normed, rate_down).astype(BF)
    learn_rate = jax.nn.sigmoid(rate_base + dot32(rate_low, rate_up))

    weight_rows = sent_together((w_receptance, w_key, w_value), "ep", 0, 1)
    reader, key_rows, value_rows = (
        dot32(normed, w).astype(BF).astype(F32) for w in weight_rows
    )
    vectors = jnp.stack(
        [
            reader,
            key_rows,
            value_rows,
            decay_rate,
            learn_rate,
            jnp.broadcast_to(key_scale[None, :], (rows, mix)),
        ],
        axis=1,
    ).reshape(rows, 6, heads, HEAD)
    mixed, new_state = mix_heads(vectors, head_gain, recurrent_state)
    mixed = mixed.reshape(rows, mix).astype(BF)
    residual = (tokens.astype(F32) + dot32(mixed, w_output)).astype(BF)
    second = rms_scale(residual, second_gain).astype(BF)

    halves = jnp.concatenate([second[:, :half], second[:, half:]], axis=0)
    outgoing = lax.dot_general(pick, halves, (((0,), (0,)), ((), ()))).astype(BF)
    received = lax.all_to_all(
        outgoing.reshape(devices, MOST * HALVES, half), "ep", split_axis=0, concat_axis=0, tiled=True
    ).reshape(devices * MOST * HALVES, half)
    shared = dot32(gated_units(second, shared_gate, shared_up), shared_down)

    block = 256
    blocks = devices * MOST * HALVES // block
    kept = block // HALVES
    source = jnp.arange(block, dtype=jnp.int32)
    target = jnp.arange(kept, dtype=jnp.int32)
    at = target // MOST * (MOST * HALVES) + target % MOST
    unchunk = [(at[:, None] + MOST * h == source[None, :]).astype(BF) for h in range(HALVES)]
    chunks = received.reshape(blocks, block, half)
    inputs = jnp.concatenate(
        [
            jnp.einsum("pq,bqc->bpc", u, chunks, preferred_element_type=F32).astype(BF)
            for u in unchunk
        ],
        axis=2,
    ).reshape(devices * MOST, width)
    hidden = gated_units(inputs, expert_gate[0], expert_up[0])
    hidden = hidden.reshape(blocks, kept, hidden.shape[1])
    spread = [
        jnp.einsum("pq,bpc->bqc", u, hidden, preferred_element_type=F32).astype(BF)
        for u in unchunk
    ]
    down = expert_down[0]
    produced = dot32(
        jnp.concatenate(spread, axis=2).reshape(devices * MOST * HALVES, -1),
        jnp.concatenate([down[:, :half], down[:, half:]], axis=0),
    ).astype(BF)
    returned = lax.all_to_all(
        produced.reshape(devices, MOST * HALVES, half), "ep", split_axis=0, concat_axis=0, tiled=True
    ).reshape(devices * MOST * HALVES, half)
    parts = dot32(weigh, returned).reshape(2, HALVES, rows, half)
    parts = parts[0] + parts[1]
    routed = jnp.concatenate([parts[0], parts[1]], axis=1)
    new_tokens = (residual.astype(F32) + shared + routed).astype(BF)
    return (new_tokens, new_state)


def solution(mesh):
    row = P("ep", None)
    block = P("ep", None, None)
    whole = P()
    in_specs = (
        (row, block, whole, row, row, row)
        + (whole,) * 13
        + (block, block, block, whole, whole)
    )
    return jax.shard_map(
        per_device, mesh=mesh, in_specs=in_specs, out_specs=(row, block), check_vma=False
    )
```

```python
import jax
import jax.numpy as jnp
from jax import lax
from jax.experimental import pallas as pl
from jax.experimental.pallas import tpu as pltpu
from jax.sharding import PartitionSpec as P

HEAD = 64
MOST = 4
HALVES = 2
RING = 4
CORES = 2
GROUP = 8
LANES = 128
BLOCK = 256
NORM_EPS = 1e-06
GROUP_EPS = 0.00064
BF = jnp.bfloat16
F32 = jnp.float32


def rms_scale(inputs, gain):
    widened = inputs.astype(F32)
    return (
        widened * lax.rsqrt(jnp.mean(widened * widened, axis=-1, keepdims=True) + NORM_EPS) * gain
    )


def dot32(a, b):
    return jnp.dot(a, b, preferred_element_type=F32)


def gated_units(inputs, gate_weight, up_weight):
    return (jax.nn.silu(dot32(inputs, gate_weight)) * dot32(inputs, up_weight)).astype(BF)


def high_low(x):
    high = x.astype(BF)
    return high, (x - high.astype(F32)).astype(BF)


def iota(shape, dim):
    return lax.broadcasted_iota(jnp.int32, shape, dim)


def whole(count):
    return [pl.BlockSpec(memory_space=pltpu.VMEM) for _ in range(count)]


def mix_kernel(
    sent_ref,
    decay_ref,
    learn_ref,
    scale_ref,
    gain_ref,
    state_ref,
    spread_ref,
    fold_ref,
    output_ref,
    tokens_ref,
    second_gain_ref,
    pick_ref,
    next_ref,
    residual_ref,
    second_ref,
    chunks_ref,
):
    rows, heads, lanes = state_ref.shape
    both = rows * heads
    members = sent_ref.shape[0]
    chunk = 1024
    row = iota((both, members), 0)
    member = iota((both, members), 1)
    mine = ((row // heads) == (member % rows)) & ((row % heads) // CORES == member // rows)
    owned = dot32(mine.astype(BF), sent_ref[...])
    side = (iota((both, LANES), 0) % CORES) == (iota((both, LANES), 1) // HEAD)
    first_half = iota((both, LANES), 1) < HEAD

    def part(i):
        return jnp.where(side, owned[:, i * LANES : (i + 1) * LANES], 0.0)

    def twice(x):
        return x + pltpu.roll(x, HEAD, 1)

    reader2 = twice(part(0))
    key2 = twice(part(1))
    value = part(2).astype(BF)
    decay2 = decay_ref[...]
    scaled = key2 * scale_ref[...]
    total = jnp.sum(scaled * scaled, axis=-1, keepdims=True) * 0.5
    dir2 = scaled / jnp.sqrt(total + 1.0)
    taken2 = dir2 * learn_ref[...]

    removed2 = jnp.zeros((both, LANES), F32)
    for c in range(lanes // chunk):
        pieces = []
        for j in range(chunk // LANES):
            at = c * chunk + j * LANES
            state = state_ref[:, :, at : at + LANES].reshape(both, LANES)
            pieces.append((state * dir2).astype(BF))
        removed2 = removed2 + dot32(
            jnp.concatenate(pieces, axis=1), fold_ref[c * chunk : (c + 1) * chunk, :]
        )
    high, low = high_low(removed2)
    known = jnp.where(first_half, high.astype(F32), low.astype(F32)).astype(BF)
    readout2 = jnp.zeros((both, LANES), F32)
    for c in range(lanes // chunk):
        spread = spread_ref[:, c * chunk : (c + 1) * chunk]
        removed_wide = dot32(known, spread)
        value_wide = dot32(value, spread)
        pieces = []
        for j in range(chunk // LANES):
            at = c * chunk + j * LANES
            sub = slice(j * LANES, (j + 1) * LANES)
            state = (
                state_ref[:, :, at : at + LANES].reshape(both, LANES) * decay2
                - removed_wide[:, sub] * taken2
                + value_wide[:, sub] * key2
            )
            next_ref[:, :, at : at + LANES] = state.reshape(rows, heads, LANES)
            pieces.append((state * reader2).astype(BF))
        readout2 = readout2 + dot32(
            jnp.concatenate(pieces, axis=1), fold_ref[c * chunk : (c + 1) * chunk, :]
        )
    centre = jnp.mean(readout2, axis=-1, keepdims=True)
    apart = readout2 - centre
    spread_of = jnp.mean(apart * apart, axis=-1, keepdims=True)
    mixed2 = apart * lax.rsqrt(spread_of + GROUP_EPS) * gain_ref[...]

    width = heads * HEAD
    own_head = (iota((both, width), 0) % heads) == (iota((both, width), 1) // HEAD)
    laid = jnp.where(own_head, jnp.concatenate([mixed2] * (width // LANES), axis=1), 0.0)
    collect = (iota((rows, both), 0) == iota((rows, both), 1) // heads).astype(BF)
    mixed = dot32(collect, laid.astype(BF)).astype(BF)
    residual = (tokens_ref[...].astype(F32) + dot32(mixed, output_ref[...])).astype(BF)
    second = rms_scale(residual, second_gain_ref[...]).astype(BF)
    residual_ref[...] = residual
    second_ref[...] = second
    half = second.shape[1] // HALVES
    halves = jnp.concatenate([second[:, h * half : (h + 1) * half] for h in range(HALVES)], axis=0)
    chunks_ref[...] = dot32(pick_ref[...], halves).astype(BF)


def mix_heads(sent, decay, learn, scale, gain, state_old, w_output, tokens, second_gain, pick):
    rows, heads, lanes = state_old.shape
    width = tokens.shape[1]
    lane = jnp.arange(lanes, dtype=jnp.int32)
    entry = jnp.arange(LANES, dtype=jnp.int32) % HEAD
    spread = (entry[:, None] == lane[None, :] // HEAD).astype(BF)
    fold = (lane[:, None] // HEAD == entry[None, :]).astype(BF)
    return pl.pallas_call(
        mix_kernel,
        in_specs=whole(12),
        out_specs=whole(4),
        out_shape=[
            jax.ShapeDtypeStruct(state_old.shape, F32),
            jax.ShapeDtypeStruct((rows, width), BF),
            jax.ShapeDtypeStruct((rows, width), BF),
            jax.ShapeDtypeStruct((pick.shape[0], width // HALVES), BF),
        ],
        name="mix",
    )(
        sent,
        decay,
        learn,
        scale,
        gain,
        state_old,
        spread,
        fold,
        w_output,
        tokens,
        second_gain[None, :],
        pick,
    )


def expert_kernel(chunks_ref, gate_ref, up_ref, down_ref, out_ref):
    half = chunks_ref.shape[1]
    kept = BLOCK // HALVES
    row = iota((BLOCK, BLOCK), 0)
    column = iota((BLOCK, BLOCK), 1)
    slot = row % kept
    split = (column == slot // MOST * (MOST * HALVES) + row // kept * MOST + slot % MOST).astype(BF)
    back = iota((BLOCK, BLOCK), 1)
    back_slot = back % kept
    source = back_slot // MOST * (MOST * HALVES) + back // kept * MOST + back_slot % MOST
    join = (iota((BLOCK, BLOCK), 0) == source).astype(BF)
    inputs = []
    for b in range(chunks_ref.shape[0] // BLOCK):
        apart = dot32(split, chunks_ref[b * BLOCK : (b + 1) * BLOCK, :]).astype(BF)
        inputs.append(jnp.concatenate([apart[:kept], apart[kept:]], axis=1))
    inputs = jnp.concatenate(inputs, axis=0)
    hidden = gated_units(inputs, gate_ref[...], up_ref[...])
    result = dot32(hidden, down_ref[...]).astype(BF)
    for b in range(chunks_ref.shape[0] // BLOCK):
        mine = result[b * kept : (b + 1) * kept]
        stacked = jnp.concatenate([mine[:, :half], mine[:, half:]], axis=0)
        out_ref[b * BLOCK : (b + 1) * BLOCK, :] = dot32(join, stacked).astype(BF)


def run_expert(chunks, gate, up, down):
    return pl.pallas_call(
        expert_kernel,
        in_specs=whole(4),
        out_specs=whole(1)[0],
        out_shape=jax.ShapeDtypeStruct(chunks.shape, BF),
        name="expert",
    )(chunks, gate, up, down)


def combine_kernel(weigh_ref, returned_ref, residual_ref, shared_ref, out_ref):
    rows = residual_ref.shape[0]
    half = returned_ref.shape[1]
    parts = dot32(weigh_ref[...], returned_ref[...])
    parts = parts[: HALVES * rows] + parts[HALVES * rows :]
    for h in range(HALVES):
        at = slice(h * half, (h + 1) * half)
        out_ref[:, at] = (
            residual_ref[:, at].astype(F32)
            + shared_ref[:, at]
            + parts[h * rows : (h + 1) * rows]
        ).astype(BF)


def combine(weigh, returned, residual, shared):
    return pl.pallas_call(
        combine_kernel,
        in_specs=whole(4),
        out_specs=whole(1)[0],
        out_shape=jax.ShapeDtypeStruct(residual.shape, BF),
        name="combine",
    )(weigh, returned, residual, shared)


def exchanged(x, groups=None):
    return lax.all_to_all(
        x, "ep", split_axis=0, concat_axis=0, tiled=True, axis_index_groups=groups
    )


def gathered_rows(normed, devices, me):
    rows, width = normed.shape
    core = me % CORES
    place = me // CORES % RING
    other = lax.ppermute(normed, "ep", [(d, d ^ 1) for d in range(devices)])
    pair = jnp.where(
        core == 0, jnp.stack([normed, other], axis=0), jnp.stack([other, normed], axis=0)
    )
    held = jnp.zeros((RING, CORES, rows, width), BF)
    held = lax.dynamic_update_slice(held, pair[None], (place, 0, 0, 0))
    for step in range(1, RING):
        hop = [
            (d, d // GROUP * GROUP + (d % GROUP + CORES * step) % GROUP) for d in range(devices)
        ]
        moved = lax.ppermute(pair, "ep", hop)
        held = lax.dynamic_update_slice(held, moved[None], ((place - step) % RING, 0, 0, 0))
    return held.reshape(GROUP * rows, width)


def per_device(
    tokens,
    recurrent_state,
    first_gain,
    w_receptance,
    w_key,
    w_value,
    decay_down,
    decay_up,
    decay_base,
    rate_down,
    rate_up,
    rate_base,
    key_scale,
    head_gain,
    w_output,
    second_gain,
    shared_gate,
    shared_up,
    shared_down,
    expert_gate,
    expert_up,
    expert_down,
    routes,
    route_weights,
):
    rows, width = tokens.shape
    heads = recurrent_state.shape[1]
    half = width // HALVES
    devices = lax.axis_size("ep")
    me = lax.axis_index("ep")

    columns = jnp.stack([w_receptance, w_key, w_value], axis=1).reshape(rows, 3, GROUP, LANES)
    columns = columns.transpose(2, 0, 1, 3).reshape(1, GROUP, rows, 3 * LANES)
    columns = jnp.broadcast_to(columns, (devices // GROUP,) + columns.shape[1:])
    weights = exchanged(columns.reshape(devices, rows, 3 * LANES)).reshape(width, 3 * LANES)
    normed = rms_scale(tokens, first_gain).astype(BF)
    group_rows = gathered_rows(normed, devices, me)

    own_routes = lax.dynamic_slice_in_dim(routes, me * rows, rows, 0)
    own_weights = lax.dynamic_slice_in_dim(route_weights, me * rows, rows, 0)
    place = jnp.arange(devices * MOST * HALVES, dtype=jnp.int32)
    named = own_routes[:, :, None] == (place // (MOST * HALVES))[None, None, :]
    weight = jnp.sum(jnp.where(named, own_weights[:, :, None], 0.0), axis=1)
    named = jnp.any(named, axis=1)
    order = jnp.arange(rows, dtype=jnp.int32)
    before = (order[None, :] < order[:, None]).astype(BF)
    slot = dot32(before, named.astype(BF))
    chosen = named & (slot == (place % MOST)[None, :].astype(F32))
    side = (place // MOST) % HALVES
    picks = [chosen & (side == h)[None, :] for h in range(HALVES)]
    pick = jnp.concatenate(picks, axis=0).astype(BF).T
    weigh_high, weigh_low = high_low(
        jnp.concatenate([jnp.where(p, weight, 0.0) for p in picks], axis=0)
    )
    weigh = jnp.concatenate([weigh_high, weigh_low], axis=0)

    decay_low = jnp.tanh(dot32(normed, decay_down)).astype(BF)
    decay_pre = decay_base + dot32(decay_low, decay_up)
    decay_rate = jnp.exp(-jnp.exp(-jax.nn.softplus(-decay_pre) - 0.5))
    rate_low = dot32(normed, rate_down).astype(BF)
    learn_rate = jax.nn.sigmoid(rate_base + dot32(rate_low, rate_up))

    def by_head(x):
        x = jnp.broadcast_to(x, (rows, heads * HEAD)).reshape(rows * heads, HEAD)
        return jnp.concatenate([x, x], axis=1)

    sums = dot32(group_rows, weights).astype(BF)
    around = [
        list(range(first, first + GROUP)) for first in range(0, devices, GROUP)
    ]
    sent = exchanged(sums.reshape(GROUP, rows, 3 * LANES), around)
    new_state, residual, second, outgoing = mix_heads(
        sent.reshape(GROUP * rows, 3 * LANES),
        by_head(decay_rate),
        by_head(learn_rate),
        by_head(key_scale),
        by_head(head_gain),
        recurrent_state,
        w_output,
        tokens,
        second_gain,
        pick,
    )
    received = exchanged(outgoing.reshape(devices, MOST * HALVES, half))
    shared = dot32(gated_units(second, shared_gate, shared_up), shared_down)
    produced = run_expert(
        received.reshape(devices * MOST * HALVES, half),
        expert_gate[0],
        expert_up[0],
        expert_down[0],
    )
    returned = exchanged(produced.reshape(devices, MOST * HALVES, half))
    new_tokens = combine(
        weigh, returned.reshape(devices * MOST * HALVES, half), residual, shared
    )
    return (new_tokens, new_state)


def solution(mesh):
    row = P("ep", None)
    block = P("ep", None, None)
    copied = P()
    in_specs = (
        (row, block, copied, row, row, row)
        + (copied,) * 13
        + (block, block, block, copied, copied)
    )
    return jax.shard_map(
        per_device, mesh=mesh, in_specs=in_specs, out_specs=(row, block), check_vma=False
    )
```

```python
import jax
import jax.numpy as jnp
from jax import lax
from jax.experimental import pallas as pl
from jax.experimental.pallas import tpu as pltpu
from jax.sharding import PartitionSpec as P

HEAD = 64
MOST = 4
HALVES = 2
RING = 4
CORES = 2
GROUP = 8
PLANES = 4
LANES = 128
BLOCK = 256
COLUMN = 1024
NORM_EPS = 1e-06
GROUP_EPS = 0.00064
BF = jnp.bfloat16
F32 = jnp.float32


def rms_scale(inputs, gain):
    widened = inputs.astype(F32)
    return (
        widened * lax.rsqrt(jnp.mean(widened * widened, axis=-1, keepdims=True) + NORM_EPS) * gain
    )


def dot32(a, b):
    return jnp.dot(a, b, preferred_element_type=F32)


def gated_units(inputs, gate_weight, up_weight):
    return (jax.nn.silu(dot32(inputs, gate_weight)) * dot32(inputs, up_weight)).astype(BF)


def high_low(x):
    high = x.astype(BF)
    return high, (x - high.astype(F32)).astype(BF)


def iota(shape, dim):
    return lax.broadcasted_iota(jnp.int32, shape, dim)


def whole(count):
    return [pl.BlockSpec(memory_space=pltpu.VMEM) for _ in range(count)]


def in_hbm(x):
    return pltpu.with_memory_space_constraint(x, pltpu.HBM)


def room(mib):
    return pltpu.CompilerParams(vmem_limit_bytes=mib * 2**20)


def fold_matrix(column):
    value = iota((COLUMN, LANES), 0) // HEAD + column * (COLUMN // HEAD)
    return (value == iota((COLUMN, LANES), 1) % HEAD).astype(BF)


def spread_matrix(column):
    value = iota((LANES, COLUMN), 1) // HEAD + column * (COLUMN // HEAD)
    return (value == iota((LANES, COLUMN), 0) % HEAD).astype(BF)


def prepare_kernel(
    routes_ref,
    weights_ref,
    tokens_ref,
    first_gain_ref,
    decay_down_ref,
    decay_up_ref,
    decay_base_ref,
    rate_down_ref,
    rate_up_ref,
    rate_base_ref,
    scale_ref,
    gain_ref,
    pick_ref,
    weigh_ref,
    decay_out,
    learn_out,
    scale_out,
    gain_out,
):
    rows, choices = routes_ref.shape
    total = pick_ref.shape[1]
    place = iota((rows, total), 1)
    named = jnp.zeros((rows, total), F32)
    weight = jnp.zeros((rows, total), F32)
    for j in range(choices):
        match = routes_ref[:, j : j + 1] == place // (MOST * HALVES)
        named = jnp.where(match, 1.0, named)
        weight = jnp.where(match, weights_ref[:, j : j + 1], weight)
    before = (iota((rows, rows), 1) < iota((rows, rows), 0)).astype(BF)
    slot = dot32(before, named.astype(BF))
    chosen = jnp.where(slot == (place % MOST).astype(F32), named, 0.0)
    for h in range(HALVES):
        mine = jnp.where((place // MOST) % HALVES == h, chosen, 0.0)
        pick_ref[h * rows : (h + 1) * rows, :] = mine.astype(BF)
        high, low = high_low(mine * weight)
        weigh_ref[h * rows : (h + 1) * rows, :] = high
        weigh_ref[(HALVES + h) * rows : (HALVES + h + 1) * rows, :] = low

    def onto(x, w_ref):
        return lax.dot_general(
            x, w_ref[...], (((1,), (1,)), ((), ())), preferred_element_type=F32
        )

    normed = rms_scale(tokens_ref[...], first_gain_ref[...]).astype(BF)
    decay_low = jnp.tanh(onto(normed, decay_down_ref)).astype(BF)
    decay_pre = decay_base_ref[...] + dot32(decay_low, decay_up_ref[...])
    below = jnp.maximum(-decay_pre, 0.0) + jnp.log1p(jnp.exp(-jnp.abs(decay_pre)))
    rate_low = onto(normed, rate_down_ref).astype(BF)
    learn_pre = rate_base_ref[...] + dot32(rate_low, rate_up_ref[...])

    width = scale_ref.shape[1]
    heads = width // HEAD
    both = rows * heads
    own = (iota((rows, heads, LANES), 2) // HEAD) == (iota((rows, heads, LANES), 1) % CORES)
    head = iota((rows, heads, LANES), 1)

    def by_head(x):
        laid = jnp.zeros((rows, heads, LANES), F32)
        for i in range(width // LANES):
            piece = x[:, i * LANES : (i + 1) * LANES][:, None, :]
            laid = jnp.where(own & (head // CORES == i), piece, laid)
        laid = laid.reshape(both, LANES)
        return laid + pltpu.roll(laid, HEAD, 1)

    decay_out[...] = by_head(jnp.exp(-jnp.exp(-below - 0.5)))
    learn_out[...] = by_head(jax.nn.sigmoid(learn_pre))
    scale_out[...] = by_head(jnp.broadcast_to(scale_ref[...], (rows, width)))
    gain_out[...] = by_head(jnp.broadcast_to(gain_ref[...], (rows, width)))


def prepare(total, heads, own_routes, own_weights, tokens, *others):
    rows = tokens.shape[0]
    laid = pltpu.HBM((rows * heads, LANES), F32)
    return pl.pallas_call(
        prepare_kernel,
        in_specs=whole(3 + len(others)),
        out_specs=whole(6),
        out_shape=[
            pltpu.HBM((HALVES * rows, total), BF),
            pltpu.HBM((2 * HALVES * rows, total), BF),
        ]
        + [laid] * 4,
        compiler_params=room(8),
        cost_estimate=pl.CostEstimate(flops=10**9, transcendentals=0, bytes_accessed=10**6),
        name="prepare",
    )(own_routes, own_weights, in_hbm(tokens), *(in_hbm(x) for x in others))


def slices_kernel(spot_ref, tokens_ref, gain_ref, out_ref, normed_ref):
    normed_ref[...] = rms_scale(tokens_ref[...], gain_ref[...]).astype(BF)
    depth = out_ref.shape[2]
    plane = spot_ref[0] // (RING * GROUP)
    for step in range(PLANES):
        at = pl.multiple_of((plane + step) % PLANES * depth, LANES)
        out_ref[step] = normed_ref[:, pl.ds(at, depth)]


def row_slices(spot, tokens, gain):
    rows, width = tokens.shape
    return pl.pallas_call(
        slices_kernel,
        in_specs=[pl.BlockSpec(memory_space=pltpu.SMEM)] + whole(2),
        out_specs=whole(1)[0],
        out_shape=jax.ShapeDtypeStruct((PLANES, rows, width // PLANES), BF),
        scratch_shapes=[pltpu.VMEM((rows, width), BF)],
        compiler_params=room(8),
        name="slices",
    )(spot, in_hbm(tokens), in_hbm(gain[None, :]))


def columns_kernel(receptance_ref, key_ref, value_ref, out_ref, parts_ref, piece_ref, sems):
    sources = (receptance_ref, key_ref, value_ref)
    reads = [
        pltpu.make_async_copy(s, parts_ref.at[i], sems.at[i]) for i, s in enumerate(sources)
    ]
    for read in reads:
        read.start()
    for read in reads:
        read.wait()
    for m in range(GROUP):
        at = slice(m * LANES, (m + 1) * LANES)
        piece_ref[m] = jnp.concatenate([parts_ref[i, :, at] for i in range(3)], axis=1)
    writes = [
        pltpu.make_async_copy(piece_ref, out_ref.at[pl.ds(a * GROUP, GROUP)], sems.at[3 + a])
        for a in range(out_ref.shape[0] // GROUP)
    ]
    for write in writes:
        write.start()
    for write in writes:
        write.wait()


def weight_columns(receptance, key, value, plane):
    rows = key.shape[0]
    hbm = pl.BlockSpec(memory_space=pltpu.HBM)
    return pl.pallas_call(
        columns_kernel,
        in_specs=[hbm] * 3,
        out_specs=hbm,
        out_shape=pltpu.HBM((plane, rows, 3 * LANES), BF),
        scratch_shapes=[
            pltpu.VMEM((3,) + key.shape, BF),
            pltpu.VMEM((GROUP, rows, 3 * LANES), BF),
            pltpu.SemaphoreType.DMA((3 + plane // GROUP,)),
        ],
        compiler_params=room(8),
        name="columns",
    )(in_hbm(receptance), in_hbm(key), in_hbm(value))


def project_kernel(spot_ref, same_ref, other_ref, weight_ref, out_ref):
    rows = out_ref.shape[1]
    spot = spot_ref[0]
    plane = spot // (GROUP * RING)
    place = spot // CORES % RING
    for side, ref in enumerate((same_ref, other_ref)):
        sums = dot32(ref[...], weight_ref[...]).astype(BF)
        core = (spot + side) % CORES
        for step in range(RING):
            for back in range(PLANES):
                member = (plane + PLANES - back) % PLANES * GROUP
                member = member + (place + RING - step) % RING * CORES + core
                at = (step * PLANES + back) * rows
                out_ref[member] = sums[at : at + rows]


def project(spot, same, other, weights, rows):
    return pl.pallas_call(
        project_kernel,
        in_specs=[pl.BlockSpec(memory_space=pltpu.SMEM)] + whole(3),
        out_specs=whole(1)[0],
        out_shape=pltpu.HBM((PLANES * GROUP, rows, weights.shape[1]), BF),
        compiler_params=room(16),
        name="project",
    )(spot, in_hbm(same), in_hbm(other), in_hbm(weights))


def read_kernel(
    sent_ref,
    decay_ref,
    learn_ref,
    scale_ref,
    gain_ref,
    state_ref,
    output_ref,
    tokens_ref,
    second_gain_ref,
    pick_ref,
    residual_ref,
    second_ref,
    chunks_ref,
    known_ref,
    value_ref,
    key_ref,
    taken_ref,
    held_ref,
    laid_ref,
    made_ref,
    sems,
    write_sems,
):
    rows, heads, lanes = state_ref.shape
    reads = []
    for c in range(lanes // COLUMN):
        at = pl.ds(c * COLUMN, COLUMN)
        reads.append(
            pltpu.make_async_copy(state_ref.at[:, :, at], held_ref.at[:, :, at], sems.at[c])
        )
    fetch = pltpu.make_async_copy(output_ref, laid_ref, sems.at[lanes // COLUMN])
    for read in reads:
        read.start()
    fetch.start()
    both = rows * heads
    members = sent_ref.shape[0] // PLANES
    chunk = COLUMN
    row = iota((both, members), 0)
    member = iota((both, members), 1)
    mine = ((row // heads) == (member % rows)) & ((row % heads) // CORES == member // rows)
    sent = sum(sent_ref[z * members : (z + 1) * members, :].astype(F32) for z in range(PLANES))
    owned = dot32(mine.astype(BF), sent.astype(BF))
    side = (iota((both, LANES), 0) % CORES) == (iota((both, LANES), 1) // HEAD)
    first_half = iota((both, LANES), 1) < HEAD

    def part(i):
        return jnp.where(side, owned[:, i * LANES : (i + 1) * LANES], 0.0)

    def twice(x):
        return x + pltpu.roll(x, HEAD, 1)

    def over_keys(x):
        return jnp.sum(x, axis=-1, keepdims=True) * 0.5

    reader2 = twice(part(0))
    key2 = twice(part(1))
    value = part(2)
    scaled = key2 * scale_ref[...]
    dir2 = scaled / jnp.sqrt(over_keys(scaled * scaled) + 1.0)
    taken2 = dir2 * learn_ref[...]
    kept2 = decay_ref[...] * reader2
    removed2 = jnp.zeros((both, LANES), F32)
    readout2 = jnp.zeros((both, LANES), F32)
    for c in range(lanes // chunk):
        removing, reading = [], []
        reads[c].wait()
        for j in range(chunk // LANES):
            at = c * chunk + j * LANES
            state = held_ref[:, :, at : at + LANES].reshape(both, LANES)
            removing.append((state * dir2).astype(BF))
            reading.append((state * kept2).astype(BF))
        fold = fold_matrix(c)
        removed2 = removed2 + dot32(jnp.concatenate(removing, axis=1), fold)
        readout2 = readout2 + dot32(jnp.concatenate(reading, axis=1), fold)
    readout2 = (
        readout2 - removed2 * over_keys(taken2 * reader2) + twice(value) * over_keys(key2 * reader2)
    )
    high, low = high_low(removed2)
    known_ref[...] = jnp.where(first_half, high.astype(F32), low.astype(F32)).astype(BF)
    value_ref[...] = value.astype(BF)
    key_ref[...] = key2
    taken_ref[...] = taken2

    centre = jnp.mean(readout2, axis=-1, keepdims=True)
    apart = readout2 - centre
    spread_of = jnp.mean(apart * apart, axis=-1, keepdims=True)
    mixed2 = apart * lax.rsqrt(spread_of + GROUP_EPS) * gain_ref[...]
    width = heads * HEAD
    own_head = (iota((both, width), 0) % heads) == (iota((both, width), 1) // HEAD)
    laid = jnp.where(own_head, jnp.concatenate([mixed2] * (width // LANES), axis=1), 0.0)
    collect = (iota((rows, both), 0) == iota((rows, both), 1) // heads).astype(BF)
    mixed = dot32(collect, laid.astype(BF)).astype(BF)
    fetch.wait()
    residual = (tokens_ref[...].astype(F32) + dot32(mixed, laid_ref[...])).astype(BF)
    second = rms_scale(residual, second_gain_ref[...]).astype(BF)
    residual_ref[...] = residual
    second_ref[...] = second
    half = second.shape[1] // HALVES
    halves = jnp.concatenate([second[:, h * half : (h + 1) * half] for h in range(HALVES)], axis=0)
    writes = []
    for b in range(made_ref.shape[0] // BLOCK):
        at = pl.ds(b * BLOCK, BLOCK)
        made_ref[at, :] = lax.dot_general(
            pick_ref[:, at], halves, (((0,), (0,)), ((), ())), preferred_element_type=F32
        ).astype(BF)
        write = pltpu.make_async_copy(made_ref.at[at], chunks_ref.at[at], write_sems.at[b])
        write.start()
        writes.append(write)
    for write in writes:
        write.wait()


def read_heads(sent, decay, learn, scale, gain, state, w_output, tokens, second_gain, pick):
    rows, heads, lanes = state.shape
    width = tokens.shape[1]
    both = rows * heads
    hbm = pl.BlockSpec(memory_space=pltpu.HBM)
    return pl.pallas_call(
        read_kernel,
        in_specs=whole(5) + [hbm, hbm] + whole(3),
        out_specs=whole(2) + [hbm] + whole(4),
        out_shape=[
            jax.ShapeDtypeStruct((rows, width), BF),
            jax.ShapeDtypeStruct((rows, width), BF),
            pltpu.HBM((pick.shape[1], width // HALVES), BF),
            jax.ShapeDtypeStruct((both, LANES), BF),
            jax.ShapeDtypeStruct((both, LANES), BF),
            jax.ShapeDtypeStruct((both, LANES), F32),
            jax.ShapeDtypeStruct((both, LANES), F32),
        ],
        compiler_params=room(32),
        scratch_shapes=[
            pltpu.VMEM(state.shape, F32),
            pltpu.VMEM(w_output.shape, BF),
            pltpu.VMEM((pick.shape[1], width // HALVES), BF),
            pltpu.SemaphoreType.DMA((lanes // COLUMN + 1,)),
            pltpu.SemaphoreType.DMA((pick.shape[1] // BLOCK,)),
        ],
        name="read",
    )(
        in_hbm(sent),
        in_hbm(decay),
        in_hbm(learn),
        in_hbm(scale),
        in_hbm(gain),
        in_hbm(state),
        in_hbm(w_output),
        in_hbm(tokens),
        in_hbm(second_gain[None, :]),
        in_hbm(pick),
    )


def write_kernel(known_ref, value_ref, key_ref, taken_ref, decay_ref, state_ref, out_ref):
    rows, heads, lanes = state_ref.shape
    both = rows * heads
    chunk = COLUMN
    for c in range(lanes // chunk):
        spread = spread_matrix(c)
        removed_wide = dot32(known_ref[...], spread)
        value_wide = dot32(value_ref[...], spread)
        for j in range(chunk // LANES):
            at = c * chunk + j * LANES
            sub = slice(j * LANES, (j + 1) * LANES)
            state = (
                state_ref[:, :, at : at + LANES].reshape(both, LANES) * decay_ref[...]
                - removed_wide[:, sub] * taken_ref[...]
                + value_wide[:, sub] * key_ref[...]
            )
            out_ref[:, :, at : at + LANES] = state.reshape(rows, heads, LANES)


def write_heads(known, value, key, taken, decay, state):
    return pl.pallas_call(
        write_kernel,
        in_specs=whole(6),
        out_specs=whole(1)[0],
        out_shape=jax.ShapeDtypeStruct(state.shape, F32),
        cost_estimate=pl.CostEstimate(flops=8 * 10**9, transcendentals=0, bytes_accessed=10**7),
        compiler_params=room(24),
        name="write",
    )(known, value, key, taken, decay, state)


def expert_kernel(chunks_ref, gate_ref, up_ref, down_ref, out_ref, made_ref, sems):
    half = chunks_ref.shape[1]
    kept = BLOCK // HALVES
    row = iota((BLOCK, BLOCK), 0)
    column = iota((BLOCK, BLOCK), 1)
    slot = row % kept
    split = (column == slot // MOST * (MOST * HALVES) + row // kept * MOST + slot % MOST).astype(BF)
    back = iota((BLOCK, BLOCK), 1)
    back_slot = back % kept
    source = back_slot // MOST * (MOST * HALVES) + back // kept * MOST + back_slot % MOST
    join = (iota((BLOCK, BLOCK), 0) == source).astype(BF)
    inputs = []
    for b in range(chunks_ref.shape[0] // BLOCK):
        apart = dot32(split, chunks_ref[b * BLOCK : (b + 1) * BLOCK, :]).astype(BF)
        inputs.append(jnp.concatenate([apart[:kept], apart[kept:]], axis=1))
    inputs = jnp.concatenate(inputs, axis=0)
    hidden = gated_units(inputs, gate_ref[...], up_ref[...])
    writes = []
    for b in range(chunks_ref.shape[0] // BLOCK):
        mine = dot32(hidden[b * kept : (b + 1) * kept], down_ref[...]).astype(BF)
        stacked = jnp.concatenate([mine[:, :half], mine[:, half:]], axis=0)
        at = pl.ds(b * BLOCK, BLOCK)
        made_ref[at, :] = dot32(join, stacked).astype(BF)
        write = pltpu.make_async_copy(made_ref.at[at], out_ref.at[at], sems.at[b])
        write.start()
        writes.append(write)
    for write in writes:
        write.wait()


def run_expert(chunks, gate, up, down):
    return pl.pallas_call(
        expert_kernel,
        in_specs=whole(4),
        out_specs=pl.BlockSpec(memory_space=pltpu.HBM),
        out_shape=pltpu.HBM(chunks.shape, BF),
        scratch_shapes=[
            pltpu.VMEM(chunks.shape, BF),
            pltpu.SemaphoreType.DMA((chunks.shape[0] // BLOCK,)),
        ],
        compiler_params=room(24),
        name="expert",
    )(chunks, gate, up, down)


def combine_kernel(weigh_ref, returned_ref, residual_ref, shared_ref, out_ref, held_ref, sems):
    rows = residual_ref.shape[0]
    total, half = returned_ref.shape
    blocks = [pl.ds(i * BLOCK, BLOCK) for i in range(total // BLOCK)]
    reads = [
        pltpu.make_async_copy(returned_ref.at[at], held_ref.at[at], sems.at[i])
        for i, at in enumerate(blocks)
    ]
    for read in reads:
        read.start()
    parts = jnp.zeros((weigh_ref.shape[0], half), F32)
    for at, read in zip(blocks, reads):
        read.wait()
        parts = parts + dot32(weigh_ref[:, at], held_ref[at, :])
    parts = parts[: HALVES * rows] + parts[HALVES * rows :]
    for h in range(HALVES):
        at = slice(h * half, (h + 1) * half)
        out_ref[:, at] = (
            residual_ref[:, at].astype(F32)
            + shared_ref[:, at]
            + parts[h * rows : (h + 1) * rows]
        ).astype(BF)


def combine(weigh, returned, residual, shared):
    return pl.pallas_call(
        combine_kernel,
        in_specs=whole(1) + [pl.BlockSpec(memory_space=pltpu.HBM)] + whole(2),
        out_specs=whole(1)[0],
        out_shape=jax.ShapeDtypeStruct(residual.shape, BF),
        scratch_shapes=[
            pltpu.VMEM(returned.shape, BF),
            pltpu.SemaphoreType.DMA((returned.shape[0] // BLOCK,)),
        ],
        compiler_params=room(8),
        name="combine",
    )(weigh, returned, residual, shared)


def exchanged(x, groups=None):
    return lax.all_to_all(
        x, "ep", split_axis=0, concat_axis=0, tiled=True, axis_index_groups=groups
    )


def group_slices(slices, devices):
    def hop(stride, step):
        ends = []
        for d in range(devices):
            place = d // stride % RING
            ends.append((d, d + ((place + step) % RING - place) * stride))
        return ends

    rows = [slices[0]]
    for step in range(1, PLANES):
        rows.append(lax.ppermute(slices[step], "ep", hop(GROUP * RING, step)))
    column = jnp.concatenate(rows, axis=0)
    rows = [column]
    for step in range(1, RING):
        rows.append(lax.ppermute(column, "ep", hop(CORES, step)))
    same = jnp.concatenate(rows, axis=0)
    return same, lax.ppermute(same, "ep", [(d, d ^ 1) for d in range(devices)])


def per_device(
    tokens,
    recurrent_state,
    first_gain,
    w_receptance,
    w_key,
    w_value,
    decay_down,
    decay_up,
    decay_base,
    rate_down,
    rate_up,
    rate_base,
    key_scale,
    head_gain,
    w_output,
    second_gain,
    shared_gate,
    shared_up,
    shared_down,
    expert_gate,
    expert_up,
    expert_down,
    routes,
    route_weights,
):
    rows, width = tokens.shape
    heads = recurrent_state.shape[1]
    half = width // HALVES
    devices = lax.axis_size("ep")
    me = lax.axis_index("ep")

    plane = RING * GROUP
    slices = row_slices(me[None], tokens, first_gain)
    columns = weight_columns(w_receptance, w_key, w_value, plane)
    same_z = [list(range(first, first + plane)) for first in range(0, devices, plane)]
    same_y = [
        [z * plane + y * GROUP + m for z in range(PLANES) for m in range(GROUP)]
        for y in range(RING)
    ]
    weights = exchanged(columns, same_z)
    same, other = group_slices(slices, devices)

    own_routes = lax.dynamic_slice_in_dim(routes, me * rows, rows, 0)
    own_weights = lax.dynamic_slice_in_dim(route_weights, me * rows, rows, 0)
    pick, weigh, decay, learn, scale, gain = prepare(
        devices * MOST * HALVES,
        heads,
        own_routes,
        own_weights,
        tokens,
        first_gain[None, :],
        decay_down.T,
        decay_up,
        decay_base[None, :],
        rate_down.T,
        rate_up,
        rate_base[None, :],
        key_scale[None, :],
        head_gain[None, :],
    )
    sums = project(me[None], same, other, weights.reshape(plane * rows, 3 * LANES), rows)
    sent = exchanged(sums, same_y)
    residual, second, outgoing, known, value, key, taken = read_heads(
        sent.reshape(plane * rows, 3 * LANES),
        decay,
        learn,
        scale,
        gain,
        recurrent_state,
        w_output,
        tokens,
        second_gain,
        pick,
    )
    received = exchanged(outgoing.reshape(devices, MOST * HALVES, half))
    shared = dot32(gated_units(second, shared_gate, shared_up), shared_down)
    new_state = write_heads(known, value, key, taken, decay, recurrent_state)
    produced = run_expert(
        received.reshape(devices * MOST * HALVES, half), expert_gate[0], expert_up[0], expert_down[0]
    )
    returned = exchanged(produced.reshape(devices, MOST * HALVES, half))
    new_tokens = combine(
        weigh, returned.reshape(devices * MOST * HALVES, half), residual, shared
    )
    return (new_tokens, new_state)


def solution(mesh):
    row = P("ep", None)
    block = P("ep", None, None)
    copied = P()
    in_specs = (
        (row, block, copied, row, row, row)
        + (copied,) * 13
        + (block, block, block, copied, copied)
    )
    return jax.shard_map(
        per_device, mesh=mesh, in_specs=in_specs, out_specs=(row, block), check_vma=False
    )
```

```python
import jax
import jax.numpy as jnp
from jax import lax
from jax.experimental import pallas as pl
from jax.experimental.pallas import tpu as pltpu
from jax.sharding import PartitionSpec as P


HEAD = 64
MOST = 4
HALVES = 2
RING = 4
CORES = 2
GROUP = 8
PLANES = 4
FETCHES = 4
LANES = 128
BLOCK = 256
COLUMN = 1024
NORM_EPS = 1e-06
GROUP_EPS = 0.00064
BF = jnp.bfloat16
F32 = jnp.float32


def rms_scale(inputs, gain):
    widened = inputs.astype(F32)
    return (
        widened * lax.rsqrt(jnp.mean(widened * widened, axis=-1, keepdims=True) + NORM_EPS) * gain
    )


def dot32(a, b):
    return jnp.dot(a, b, preferred_element_type=F32)


def gated_units(inputs, gate_weight, up_weight):
    return (jax.nn.silu(dot32(inputs, gate_weight)) * dot32(inputs, up_weight)).astype(BF)


def high_low(x):
    high = x.astype(BF)
    return high, (x - high.astype(F32)).astype(BF)


def iota(shape, dim):
    return lax.broadcasted_iota(jnp.int32, shape, dim)


def whole(count):
    return [pl.BlockSpec(memory_space=pltpu.VMEM) for _ in range(count)]


def in_hbm(x):
    return pltpu.with_memory_space_constraint(x, pltpu.HBM)


def room(mib):
    return pltpu.CompilerParams(vmem_limit_bytes=mib * 2**20)


def fold_matrix(column):
    value = iota((COLUMN, LANES), 0) // HEAD + column * (COLUMN // HEAD)
    return (value == iota((COLUMN, LANES), 1) % HEAD).astype(BF)


def spread_matrix(column):
    value = iota((LANES, COLUMN), 1) // HEAD + column * (COLUMN // HEAD)
    return (value == iota((LANES, COLUMN), 0) % HEAD).astype(BF)


def prepare_kernel(
    spot_ref,
    routes_ref,
    weights_ref,
    tokens_ref,
    first_gain_ref,
    decay_down_ref,
    decay_up_ref,
    decay_base_ref,
    rate_down_ref,
    rate_up_ref,
    rate_base_ref,
    scale_ref,
    gain_ref,
    pick_ref,
    weigh_ref,
    decay_out,
    learn_out,
    scale_out,
    gain_out,
    routes_held,
    weights_held,
    sems,
):
    rows = tokens_ref.shape[0]
    choices = routes_ref.shape[0]
    shared = LANES // rows
    spot = spot_ref[0]
    at = pl.ds(pl.multiple_of(spot // shared * LANES, LANES), LANES)
    reads = [
        pltpu.make_async_copy(routes_ref.at[:, at], routes_held, sems.at[0]),
        pltpu.make_async_copy(weights_ref.at[:, at], weights_held, sems.at[1]),
    ]
    for read in reads:
        read.start()
    for read in reads:
        read.wait()
    total = pick_ref.shape[1]
    both_held = jnp.concatenate([routes_held[...].astype(F32), weights_held[...]], axis=0)
    mine = iota((LANES, rows), 0) == iota((LANES, rows), 1) + spot % shared * rows
    own = lax.dot_general(
        mine.astype(F32),
        both_held,
        (((0,), (1,)), ((), ())),
        precision=lax.Precision.HIGHEST,
        preferred_element_type=F32,
    )
    place = iota((rows, total), 1)
    expert = (place // (MOST * HALVES)).astype(F32)
    named = jnp.zeros((rows, total), F32)
    weight = jnp.zeros((rows, total), F32)
    for j in range(choices):
        match = own[:, j : j + 1] == expert
        named = jnp.where(match, 1.0, named)
        weight = jnp.where(match, own[:, choices + j : choices + j + 1], weight)
    before = (iota((rows, rows), 1) < iota((rows, rows), 0)).astype(BF)
    slot = dot32(before, named.astype(BF))
    chosen = jnp.where(slot == (place % MOST).astype(F32), named, 0.0)
    for h in range(HALVES):
        mine = jnp.where((place // MOST) % HALVES == h, chosen, 0.0)
        pick_ref[h * rows : (h + 1) * rows, :] = mine.astype(BF)
        high, low = high_low(mine * weight)
        weigh_ref[h * rows : (h + 1) * rows, :] = high
        weigh_ref[(HALVES + h) * rows : (HALVES + h + 1) * rows, :] = low

    def onto(x, w_ref):
        return lax.dot_general(
            x, w_ref[...], (((1,), (1,)), ((), ())), preferred_element_type=F32
        )

    normed = rms_scale(tokens_ref[...], first_gain_ref[...]).astype(BF)
    decay_low = jnp.tanh(onto(normed, decay_down_ref)).astype(BF)
    decay_pre = decay_base_ref[...] + dot32(decay_low, decay_up_ref[...])
    below = jnp.maximum(-decay_pre, 0.0) + jnp.log1p(jnp.exp(-jnp.abs(decay_pre)))
    rate_low = onto(normed, rate_down_ref).astype(BF)
    learn_pre = rate_base_ref[...] + dot32(rate_low, rate_up_ref[...])

    width = scale_ref.shape[1]
    heads = width // HEAD
    both = rows * heads
    ours = (iota((rows, heads, LANES), 2) // HEAD) == (iota((rows, heads, LANES), 1) % CORES)
    head = iota((rows, heads, LANES), 1)

    def by_head(x):
        laid = jnp.zeros((rows, heads, LANES), F32)
        for i in range(width // LANES):
            piece = x[:, i * LANES : (i + 1) * LANES][:, None, :]
            laid = jnp.where(ours & (head // CORES == i), piece, laid)
        laid = laid.reshape(both, LANES)
        return laid + pltpu.roll(laid, HEAD, 1)

    decay_out[...] = by_head(jnp.exp(-jnp.exp(-below - 0.5)))
    learn_out[...] = by_head(jax.nn.sigmoid(learn_pre))
    scale_out[...] = by_head(jnp.broadcast_to(scale_ref[...], (rows, width)))
    gain_out[...] = by_head(jnp.broadcast_to(gain_ref[...], (rows, width)))


def prepare(total, heads, spot, routes, weights, tokens, *others):
    rows = tokens.shape[0]
    hbm = pl.BlockSpec(memory_space=pltpu.HBM)
    laid = jax.ShapeDtypeStruct((rows * heads, LANES), F32)
    return pl.pallas_call(
        prepare_kernel,
        in_specs=[pl.BlockSpec(memory_space=pltpu.SMEM), hbm, hbm] + whole(1 + len(others)),
        out_specs=whole(6),
        out_shape=[
            jax.ShapeDtypeStruct((HALVES * rows, total), BF),
            pltpu.HBM((2 * HALVES * rows, total), BF),
        ]
        + [laid] * 4,
        compiler_params=room(8),
        scratch_shapes=[
            pltpu.VMEM((routes.shape[0], LANES), jnp.int32),
            pltpu.VMEM((routes.shape[0], LANES), F32),
            pltpu.SemaphoreType.DMA((2,)),
        ],
        name="prepare",
    )(spot, in_hbm(routes), in_hbm(weights), in_hbm(tokens), *(in_hbm(x) for x in others))


def slices_kernel(spot_ref, tokens_ref, gain_ref, out_ref, normed_ref):
    normed_ref[...] = rms_scale(tokens_ref[...], gain_ref[...]).astype(BF)
    depth = out_ref.shape[2]
    plane = spot_ref[0] // (RING * GROUP)
    for step in range(PLANES):
        at = pl.multiple_of((plane + step) % PLANES * depth, LANES)
        out_ref[step] = normed_ref[:, pl.ds(at, depth)]


def row_slices(spot, tokens, gain):
    rows, width = tokens.shape
    return pl.pallas_call(
        slices_kernel,
        in_specs=[pl.BlockSpec(memory_space=pltpu.SMEM)] + whole(2),
        out_specs=whole(1)[0],
        out_shape=jax.ShapeDtypeStruct((PLANES, rows, width // PLANES), BF),
        scratch_shapes=[pltpu.VMEM((rows, width), BF)],
        compiler_params=room(8),
        name="slices",
    )(spot, in_hbm(tokens), in_hbm(gain[None, :]))


def columns_kernel(receptance_ref, key_ref, value_ref, out_ref, parts_ref, piece_ref, sems):
    sources = (receptance_ref, key_ref, value_ref)
    reads = [
        pltpu.make_async_copy(s, parts_ref.at[i], sems.at[i]) for i, s in enumerate(sources)
    ]
    for read in reads:
        read.start()
    for read in reads:
        read.wait()
    for m in range(GROUP):
        at = slice(m * LANES, (m + 1) * LANES)
        piece_ref[m] = jnp.concatenate([parts_ref[i, :, at] for i in range(3)], axis=1)
    writes = [
        pltpu.make_async_copy(piece_ref, out_ref.at[pl.ds(a * GROUP, GROUP)], sems.at[3 + a])
        for a in range(out_ref.shape[0] // GROUP)
    ]
    for write in writes:
        write.start()
    for write in writes:
        write.wait()


def weight_columns(receptance, key, value, plane):
    rows = key.shape[0]
    hbm = pl.BlockSpec(memory_space=pltpu.HBM)
    return pl.pallas_call(
        columns_kernel,
        in_specs=[hbm] * 3,
        out_specs=hbm,
        out_shape=pltpu.HBM((plane, rows, 3 * LANES), BF),
        scratch_shapes=[
            pltpu.VMEM((3,) + key.shape, BF),
            pltpu.VMEM((GROUP, rows, 3 * LANES), BF),
            pltpu.SemaphoreType.DMA((3 + plane // GROUP,)),
        ],
        compiler_params=room(8),
        name="columns",
    )(in_hbm(receptance), in_hbm(key), in_hbm(value))


def project_kernel(
    spot_ref,
    same_ref,
    other_ref,
    weight_ref,
    state_ref,
    output_ref,
    out_ref,
    held_ref,
    laid_ref,
    sems,
):
    fetches = []
    for source, target in ((state_ref, held_ref), (output_ref, laid_ref)):
        size = source.shape[0] // FETCHES
        for i in range(FETCHES):
            at = pl.ds(i * size, size)
            fetches.append(
                pltpu.make_async_copy(source.at[at], target.at[at], sems.at[len(fetches)])
            )
    for fetch in fetches:
        fetch.start()
    rows = out_ref.shape[1]
    spot = spot_ref[0]
    plane = spot // (GROUP * RING)
    place = spot // CORES % RING
    for side, ref in enumerate((same_ref, other_ref)):
        sums = dot32(ref[...], weight_ref[...]).astype(BF)
        core = (spot + side) % CORES
        for step in range(RING):
            for back in range(PLANES):
                member = (plane + PLANES - back) % PLANES * GROUP
                member = member + (place + RING - step) % RING * CORES + core
                at = (step * PLANES + back) * rows
                out_ref[member] = sums[at : at + rows]
    for fetch in fetches:
        fetch.wait()


def project(spot, same, other, weights, state, w_output, rows):
    hbm = pl.BlockSpec(memory_space=pltpu.HBM)
    return pl.pallas_call(
        project_kernel,
        in_specs=[pl.BlockSpec(memory_space=pltpu.SMEM)] + whole(3) + [hbm] * 2,
        out_specs=whole(3),
        out_shape=[
            jax.ShapeDtypeStruct((PLANES * GROUP, rows, weights.shape[1]), BF),
            pltpu.VMEM(state.shape, F32),
            pltpu.VMEM(w_output.shape, BF),
        ],
        scratch_shapes=[pltpu.SemaphoreType.DMA((2 * FETCHES,))],
        compiler_params=room(8),
        name="project",
    )(spot, same, other, weights, in_hbm(state), in_hbm(w_output))


def read_kernel(
    sent_ref,
    decay_ref,
    learn_ref,
    scale_ref,
    gain_ref,
    state_ref,
    output_ref,
    tokens_ref,
    second_gain_ref,
    pick_ref,
    residual_ref,
    second_ref,
    chunks_ref,
    known_ref,
    value_ref,
    key_ref,
    taken_ref,
):
    rows, heads, lanes = state_ref.shape
    both = rows * heads
    members = sent_ref.shape[0] // PLANES
    chunk = COLUMN
    row = iota((both, members), 0)
    member = iota((both, members), 1)
    mine = ((row // heads) == (member % rows)) & ((row % heads) // CORES == member // rows)
    sent = sum(sent_ref[z * members : (z + 1) * members, :].astype(F32) for z in range(PLANES))
    owned = dot32(mine.astype(BF), sent.astype(BF))
    side = (iota((both, LANES), 0) % CORES) == (iota((both, LANES), 1) // HEAD)
    first_half = iota((both, LANES), 1) < HEAD

    def part(i):
        return jnp.where(side, owned[:, i * LANES : (i + 1) * LANES], 0.0)

    def twice(x):
        return x + pltpu.roll(x, HEAD, 1)

    def over_keys(x):
        return jnp.sum(x, axis=-1, keepdims=True) * 0.5

    reader2 = twice(part(0))
    key2 = twice(part(1))
    value = part(2)
    scaled = key2 * scale_ref[...]
    dir2 = scaled / jnp.sqrt(over_keys(scaled * scaled) + 1.0)
    taken2 = dir2 * learn_ref[...]
    kept2 = decay_ref[...] * reader2
    removed2 = jnp.zeros((both, LANES), F32)
    readout2 = jnp.zeros((both, LANES), F32)
    for c in range(lanes // chunk):
        removing, reading = [], []
        for j in range(chunk // LANES):
            at = c * chunk + j * LANES
            state = state_ref[:, :, at : at + LANES].reshape(both, LANES)
            removing.append((state * dir2).astype(BF))
            reading.append((state * kept2).astype(BF))
        fold = fold_matrix(c)
        removed2 = removed2 + dot32(jnp.concatenate(removing, axis=1), fold)
        readout2 = readout2 + dot32(jnp.concatenate(reading, axis=1), fold)
    readout2 = (
        readout2 - removed2 * over_keys(taken2 * reader2) + twice(value) * over_keys(key2 * reader2)
    )
    high, low = high_low(removed2)
    known_ref[...] = jnp.where(first_half, high.astype(F32), low.astype(F32)).astype(BF)
    value_ref[...] = value.astype(BF)
    key_ref[...] = key2
    taken_ref[...] = taken2

    centre = jnp.mean(readout2, axis=-1, keepdims=True)
    apart = readout2 - centre
    spread_of = jnp.mean(apart * apart, axis=-1, keepdims=True)
    mixed2 = apart * lax.rsqrt(spread_of + GROUP_EPS) * gain_ref[...]
    width = heads * HEAD
    own_head = (iota((both, width), 0) % heads) == (iota((both, width), 1) // HEAD)
    laid = jnp.where(own_head, jnp.concatenate([mixed2] * (width // LANES), axis=1), 0.0)
    collect = (iota((rows, both), 0) == iota((rows, both), 1) // heads).astype(BF)
    mixed = dot32(collect, laid.astype(BF)).astype(BF)
    residual = (tokens_ref[...].astype(F32) + dot32(mixed, output_ref[...])).astype(BF)
    second = rms_scale(residual, second_gain_ref[...]).astype(BF)
    residual_ref[...] = residual
    second_ref[...] = second
    half = second.shape[1] // HALVES
    halves = jnp.concatenate([second[:, h * half : (h + 1) * half] for h in range(HALVES)], axis=0)
    chunks_ref[...] = lax.dot_general(
        pick_ref[...], halves, (((0,), (0,)), ((), ())), preferred_element_type=F32
    ).astype(BF)


def read_heads(sent, decay, learn, scale, gain, state, w_output, tokens, second_gain, pick):
    rows, heads, _ = state.shape
    width = tokens.shape[1]
    both = rows * heads
    hbm = pl.BlockSpec(memory_space=pltpu.HBM)
    return pl.pallas_call(
        read_kernel,
        in_specs=whole(10),
        out_specs=whole(7),
        out_shape=[
            jax.ShapeDtypeStruct((rows, width), BF),
            jax.ShapeDtypeStruct((rows, width), BF),
            jax.ShapeDtypeStruct((pick.shape[1], width // HALVES), BF),
            jax.ShapeDtypeStruct((both, LANES), BF),
            jax.ShapeDtypeStruct((both, LANES), BF),
            jax.ShapeDtypeStruct((both, LANES), F32),
            jax.ShapeDtypeStruct((both, LANES), F32),
        ],
        compiler_params=room(24),
        name="read",
    )(
        sent,
        decay,
        learn,
        scale,
        gain,
        state,
        w_output,
        in_hbm(tokens),
        in_hbm(second_gain[None, :]),
        pick,
    )


def write_kernel(known_ref, value_ref, key_ref, taken_ref, decay_ref, state_ref, out_ref):
    rows, heads, lanes = state_ref.shape
    both = rows * heads
    chunk = COLUMN
    for c in range(lanes // chunk):
        spread = spread_matrix(c)
        removed_wide = dot32(known_ref[...], spread)
        value_wide = dot32(value_ref[...], spread)
        for j in range(chunk // LANES):
            at = c * chunk + j * LANES
            sub = slice(j * LANES, (j + 1) * LANES)
            state = (
                state_ref[:, :, at : at + LANES].reshape(both, LANES) * decay_ref[...]
                - removed_wide[:, sub] * taken_ref[...]
                + value_wide[:, sub] * key_ref[...]
            )
            out_ref[:, :, at : at + LANES] = state.reshape(rows, heads, LANES)


def write_heads(known, value, key, taken, decay, state):
    return pl.pallas_call(
        write_kernel,
        in_specs=whole(6),
        out_specs=whole(1)[0],
        out_shape=jax.ShapeDtypeStruct(state.shape, F32),
        cost_estimate=pl.CostEstimate(flops=8 * 10**9, transcendentals=0, bytes_accessed=10**7),
        compiler_params=room(24),
        name="write",
    )(known, value, key, taken, decay, state)


def expert_kernel(chunks_ref, gate_ref, up_ref, down_ref, out_ref, made_ref, sems):
    half = chunks_ref.shape[1]
    kept = BLOCK // HALVES
    row = iota((BLOCK, BLOCK), 0)
    column = iota((BLOCK, BLOCK), 1)
    slot = row % kept
    split = (column == slot // MOST * (MOST * HALVES) + row // kept * MOST + slot % MOST).astype(BF)
    back = iota((BLOCK, BLOCK), 1)
    back_slot = back % kept
    source = back_slot // MOST * (MOST * HALVES) + back // kept * MOST + back_slot % MOST
    join = (iota((BLOCK, BLOCK), 0) == source).astype(BF)
    blocks = chunks_ref.shape[0] // BLOCK
    writes = []
    for first in range(0, blocks, blocks // 2):
        span = range(first, first + blocks // 2)
        inputs = []
        for b in span:
            apart = dot32(split, chunks_ref[b * BLOCK : (b + 1) * BLOCK, :]).astype(BF)
            inputs.append(jnp.concatenate([apart[:kept], apart[kept:]], axis=1))
        hidden = gated_units(jnp.concatenate(inputs, axis=0), gate_ref[...], up_ref[...])
        made = dot32(hidden, down_ref[...]).astype(BF)
        for i, b in enumerate(span):
            mine = made[i * kept : (i + 1) * kept]
            stacked = jnp.concatenate([mine[:, :half], mine[:, half:]], axis=0)
            at = pl.ds(b * BLOCK, BLOCK)
            made_ref[at, :] = dot32(join, stacked).astype(BF)
            write = pltpu.make_async_copy(made_ref.at[at], out_ref.at[at], sems.at[b])
            write.start()
            writes.append(write)
    for write in writes:
        write.wait()


def run_expert(chunks, gate, up, down):
    return pl.pallas_call(
        expert_kernel,
        in_specs=whole(4),
        out_specs=pl.BlockSpec(memory_space=pltpu.HBM),
        out_shape=pltpu.HBM(chunks.shape, BF),
        scratch_shapes=[
            pltpu.VMEM(chunks.shape, BF),
            pltpu.SemaphoreType.DMA((chunks.shape[0] // BLOCK,)),
        ],
        compiler_params=room(24),
        name="expert",
    )(chunks, gate, up, down)


def combine_kernel(weigh_ref, returned_ref, residual_ref, shared_ref, out_ref, held_ref, sems):
    rows = residual_ref.shape[0]
    total, half = returned_ref.shape
    blocks = [pl.ds(i * BLOCK, BLOCK) for i in range(total // BLOCK)]
    reads = [
        pltpu.make_async_copy(returned_ref.at[at], held_ref.at[at], sems.at[i])
        for i, at in enumerate(blocks)
    ]
    for read in reads:
        read.start()
    parts = jnp.zeros((weigh_ref.shape[0], half), F32)
    for at, read in zip(blocks, reads):
        read.wait()
        parts = parts + dot32(weigh_ref[:, at], held_ref[at, :])
    parts = parts[: HALVES * rows] + parts[HALVES * rows :]
    for h in range(HALVES):
        at = slice(h * half, (h + 1) * half)
        out_ref[:, at] = (
            residual_ref[:, at].astype(F32)
            + shared_ref[:, at]
            + parts[h * rows : (h + 1) * rows]
        ).astype(BF)


def combine(weigh, returned, residual, shared):
    return pl.pallas_call(
        combine_kernel,
        in_specs=whole(1) + [pl.BlockSpec(memory_space=pltpu.HBM)] + whole(2),
        out_specs=whole(1)[0],
        out_shape=jax.ShapeDtypeStruct(residual.shape, BF),
        scratch_shapes=[
            pltpu.VMEM(returned.shape, BF),
            pltpu.SemaphoreType.DMA((returned.shape[0] // BLOCK,)),
        ],
        compiler_params=room(8),
        name="combine",
    )(weigh, returned, residual, shared)


def exchanged(x, groups=None):
    return lax.all_to_all(
        x, "ep", split_axis=0, concat_axis=0, tiled=True, axis_index_groups=groups
    )


def group_slices(slices, devices):
    def hop(stride, step):
        ends = []
        for d in range(devices):
            place = d // stride % RING
            ends.append((d, d + ((place + step) % RING - place) * stride))
        return ends

    rows = [slices[0]]
    for step in range(1, PLANES):
        rows.append(lax.ppermute(slices[step], "ep", hop(GROUP * RING, step)))
    column = jnp.concatenate(rows, axis=0)
    rows = [column]
    for step in range(1, RING):
        rows.append(lax.ppermute(column, "ep", hop(CORES, step)))
    return jnp.concatenate(rows, axis=0)


def per_device(
    tokens,
    recurrent_state,
    first_gain,
    w_receptance,
    w_key,
    w_value,
    decay_down,
    decay_up,
    decay_base,
    rate_down,
    rate_up,
    rate_base,
    key_scale,
    head_gain,
    w_output,
    second_gain,
    shared_gate,
    shared_up,
    shared_down,
    expert_gate,
    expert_up,
    expert_down,
    routes,
    route_weights,
):
    rows, width = tokens.shape
    heads = recurrent_state.shape[1]
    half = width // HALVES
    devices = lax.axis_size("ep")
    me = lax.axis_index("ep")

    plane = RING * GROUP
    slices = row_slices(me[None], tokens, first_gain)
    columns = weight_columns(w_receptance, w_key, w_value, plane)
    same_z = [list(range(first, first + plane)) for first in range(0, devices, plane)]
    same_y = [
        [z * plane + y * GROUP + m for z in range(PLANES) for m in range(GROUP)]
        for y in range(RING)
    ]
    weights = exchanged(columns, same_z)
    same = group_slices(slices, devices)

    pick, weigh, decay, learn, scale, gain = prepare(
        devices * MOST * HALVES,
        heads,
        me[None],
        routes.T,
        route_weights.T,
        tokens,
        first_gain[None, :],
        decay_down.T,
        decay_up,
        decay_base[None, :],
        rate_down.T,
        rate_up,
        rate_base[None, :],
        key_scale[None, :],
        head_gain[None, :],
    )
    same, pick, weigh, decay, learn, scale, gain = lax.optimization_barrier(
        (same, pick, weigh, decay, learn, scale, gain)
    )
    other = lax.ppermute(same, "ep", [(d, d ^ 1) for d in range(devices)])
    sums, state, output_weight = project(
        me[None],
        same,
        other,
        weights.reshape(plane * rows, 3 * LANES),
        recurrent_state,
        w_output,
        rows,
    )
    sent = exchanged(sums, same_y)
    residual, second, outgoing, known, value, key, taken = read_heads(
        sent.reshape(plane * rows, 3 * LANES),
        decay,
        learn,
        scale,
        gain,
        state,
        output_weight,
        tokens,
        second_gain,
        pick,
    )
    received = exchanged(outgoing.reshape(devices, MOST * HALVES, half))
    shared = dot32(gated_units(second, shared_gate, shared_up), shared_down)
    new_state = write_heads(known, value, key, taken, decay, recurrent_state)
    produced = run_expert(
        received.reshape(devices * MOST * HALVES, half), expert_gate[0], expert_up[0], expert_down[0]
    )
    returned = exchanged(produced.reshape(devices, MOST * HALVES, half))
    new_tokens = combine(
        weigh, returned.reshape(devices * MOST * HALVES, half), residual, shared
    )
    return (new_tokens, new_state)


def solution(mesh):
    row = P("ep", None)
    block = P("ep", None, None)
    copied = P()
    in_specs = (
        (row, block, copied, row, row, row)
        + (copied,) * 13
        + (block, block, block, copied, copied)
    )
    return jax.shard_map(
        per_device, mesh=mesh, in_specs=in_specs, out_specs=(row, block), check_vma=False
    )
```
